32 devices in a mesh: ep: 8 (over z, x), tp: 4 (over y, core).
Axes of the slice: x: 2, y: 2, z: 4, core: 2. Of those that a mesh axis runs over, the one named last changes fastest.
Arguments:
- tokens: bfloat16 [768, 4096], P('ep'), may hold values from -6 to 6
- mix_gain: float32 [4096], replicated, may hold values from 0.1 to 1.9
- ffn_gain: float32 [4096], replicated, may hold values from 0.1 to 1.9
- in_proj: bfloat16 [4096, 1024], P(None, 'tp'), may hold values from -0.09375 to 0.09375
- decay_rate: float32 [64, 64], P('tp'), may hold values from 0.05 to 2
- frequency: float32 [64, 64], P('tp'), may hold values from -3 to 3
- log_step: float32 [64], P('tp'), may hold values from -3 to 0.5
- b_real: float32 [64, 64, 16], P('tp'), may hold values from -1.5 to 1.5
- b_imag: float32 [64, 64, 16], P('tp'), may hold values from -1.5 to 1.5
- c_real: float32 [64, 16, 64], P('tp'), may hold values from -0.75 to 0.75
- c_imag: float32 [64, 16, 64], P('tp'), may hold values from -0.75 to 0.75
- skip_gain: float32 [1024], P('tp'), may hold values from -5 to 5
- states: float32 [2, 768, 4096], P(None, 'ep', 'tp'), may hold values from -6 to 6
- out_proj: bfloat16 [1024, 4096], P('tp'), may hold values from -0.1875 to 0.1875
- route_ids: int32 [768, 2], P('ep'), may hold values from 0 to 7, all different within a row; in each aligned block of 96 rows (0 to 95, 96 to 191, ...) at most 48 rows name the same one
- route_logits: float32 [768, 2], P('ep'), may hold values from -5 to 5
- expert_gate: bfloat16 [8, 4096, 3072], P('ep', None, 'tp'), may hold values from -0.09375 to 0.09375
- expert_up: bfloat16 [8, 4096, 3072], P('ep', None, 'tp'), may hold values from -0.09375 to 0.09375
- expert_down: bfloat16 [8, 3072, 4096], P('ep', 'tp'), may hold values from -0.109375 to 0.109375
- dense_gate: bfloat16 [4096, 6144], P('tp', 'ep'), may hold values from -0.09375 to 0.09375
- dense_up: bfloat16 [4096, 6144], P('tp', 'ep'), may hold values from -0.09375 to 0.09375
- dense_down: bfloat16 [6144, 4096], P('ep', 'tp'), may hold values from -0.078125 to 0.078125
- branch_gate: bfloat16 [4096], replicated, may hold values from -0.09375 to 0.09375
Outputs:
- output: bfloat16 [768, 4096], P('ep', 'tp')
- new_states: float32 [2, 768, 4096], P(None, 'ep', 'tp')
The draws below stay inside these ranges and needn't reach their ends.
Inputs may be any that keep to these rules, and one draw needn't show every extreme that they name: `route_ids`: each row names 2 different experts; among the rows of one device (aligned blocks of 96 rows) no expert is named by more than 48 rows.
All inputs are finite; a program needn't handle non-finite values.
Results may differ from the reference program's by a relative error of at most 0.017.
Values may be sent and summed in bfloat16 or wider, within the bound.
A program may use at most 128 MiB of HBM per device.

```python
import math
import jax
import jax.numpy as jnp
import numpy as np
from jax import lax

D = 4096
S5W = 1024
GROUP = 16
GROUPS = 64
STATE = 64
FFE = 3072
FFD = 6144
TOPK = 2
SEQ_DEV = 96
BATCH = 768
EXPERTS = 8
CAP = 48
N_EP = 8
N_TP = 4


def steps_of(own_key, dims, cuts, least, top_value):
    loudness, own = 1.0, jax.random.fold_in(own_key, 6)
    for axis_at, blocks in cuts:
        steps = jnp.exp(jax.random.uniform(jax.random.fold_in(own, axis_at), (blocks,), jnp.float32, least / len(cuts), top_value / len(cuts)))
        loudness = loudness * jnp.repeat(steps, dims[axis_at] // blocks).reshape([-1 if axis == axis_at else 1 for axis in range(len(dims))])
    return loudness


def deal_out(key, own, number, rows, number_of, top, bound, slope):
    sequence = jax.random.permutation(key, number_of)
    crowded, ordinary = portions_of(number_of, rows * top, bound, slope, True), portions_of(number_of, rows * top, bound, slope, False)
    places = jnp.arange(number_of)

    def named(lengths, turn):
        used = int((lengths > 0).sum())
        fixed = max(1, used // 4)
        passed = fixed + (places - fixed + turn * (used - fixed)) % max(1, number_of - fixed)
        return jnp.zeros((number_of,), jnp.int32).at[sequence[jnp.where(places < fixed, places, passed)]].set(jnp.asarray(lengths, jnp.int32))

    lengths = jnp.where(number % 4 == 0, named(crowded, number // 4), named(ordinary, number - number // 4 - 1))
    mixed = jax.random.permutation(jax.random.fold_in(own, 3), number_of)
    donor, receiver = mixed[0:number_of // 2 * 2:2], mixed[1:number_of // 2 * 2:2]
    slack = jnp.minimum(lengths[donor] - 1, bound - lengths[receiver]) // 2
    slack = jnp.where((donor == sequence[0]) | (receiver == sequence[0]) | (lengths[receiver] == 0), 0, jnp.maximum(slack, 0))
    passed = jax.random.randint(jax.random.fold_in(own, 4), (number_of // 2,), 0, 1 << 20) % (slack + 1)
    lengths = lengths.at[donor].add(-passed).at[receiver].add(passed)
    labels = jnp.searchsorted(jnp.cumsum(lengths), jnp.arange(rows * top), side="right").astype(jnp.int32)
    listing = labels.reshape(top, rows).T
    listing = listing[jax.random.permutation(jax.random.fold_in(own, 1), rows)]
    turn = jax.random.randint(jax.random.fold_in(own, 2), (rows, 1), 0, top)
    return jnp.take_along_axis(listing, (jnp.arange(top)[None, :] + turn) % top, axis=1)


def portions_of(amount, total, bound, slope, full):
    weights = [(1 << 20) // math.isqrt(standing ** slope) + 1 for standing in range(1, amount + 1)]
    largest = bound if full else min(bound, max(-(-total // amount), total * weights[0] // sum(weights)))
    least = 1 if total - largest >= amount - 1 else 0
    counts, rest = [largest] + [least] * (amount - 1), total - largest - least * (amount - 1)
    while rest > 0:
        free = [i for i in range(1, amount) if counts[i] < largest] or [i for i in range(1, amount) if counts[i] < bound]
        mass, budget = sum([weights[i] for i in free]), rest
        for i in free:
            addition = min(bound - counts[i], max(1, budget * weights[i] // mass), rest)
            counts[i] = counts[i] + addition
            rest = rest - addition
    return np.array(counts)


def noise(rng, extent, width, bound, pieces=(), kind=jnp.bfloat16):
    loudness = steps_of(rng, extent, pieces, -0.22, 0.18) if pieces else 1.0
    values = jax.random.normal(rng, extent, jnp.float32) * width * loudness
    return jnp.minimum(jnp.maximum(values, -bound), bound).astype(kind)


def setup_inputs(seed: int = 0) -> dict:
    seeds = jax.random.split(jax.random.key(seed), 24)
    tokens = noise(seeds[0], (BATCH, D), 1.0, 6.0, ((0, 8),))
    mix_gain = jnp.clip(1.0 + 0.18 * jax.random.normal(seeds[1], (D,), jnp.float32), 0.1, 1.9)
    ffn_gain = jnp.clip(1.0 + 0.18 * jax.random.normal(seeds[2], (D,), jnp.float32), 0.1, 1.9)
    in_proj = noise(seeds[3], (D, S5W), D ** -0.5, 0.09375, ((1, 4),))
    decay_rate = jnp.clip(jnp.exp(math.log(2.0) - 3.6888794 * jax.random.uniform(seeds[4], (GROUPS, STATE), jnp.float32) ** steps_of(seeds[4], (GROUPS, STATE), ((0, 4),), -0.2, 0.2)), 0.05, 2.0)
    frequency = jnp.clip(jax.random.uniform(seeds[5], (GROUPS, STATE), jnp.float32, -3.0, 3.0) * steps_of(seeds[5], (GROUPS, STATE), ((0, 4),), -0.4, 0.0), -3.0, 3.0)
    log_step = jnp.clip(-3.0 + 3.5 * jax.random.uniform(seeds[6], (GROUPS,), jnp.float32) ** steps_of(seeds[6], (GROUPS,), ((0, 4),), -0.2, 0.2), -3.0, 0.5)
    b_real = noise(seeds[7], (GROUPS, STATE, GROUP), GROUP ** -0.5, 1.5, ((0, 4),), jnp.float32)
    b_imag = noise(seeds[8], (GROUPS, STATE, GROUP), GROUP ** -0.5, 1.5, ((0, 4),), jnp.float32)
    c_real = noise(seeds[9], (GROUPS, GROUP, STATE), STATE ** -0.5, 0.75, ((0, 4),), jnp.float32)
    c_imag = noise(seeds[10], (GROUPS, GROUP, STATE), STATE ** -0.5, 0.75, ((0, 4),), jnp.float32)
    skip_gain = noise(seeds[11], (S5W,), 1.0, 5.0, ((0, 4),), jnp.float32)
    states = noise(seeds[12], (2, BATCH, GROUPS * STATE), 1.0, 6.0, ((1, 8), (2, 4)), jnp.float32)
    out_proj = noise(seeds[13], (S5W, D), S5W ** -0.5, 0.1875, ((0, 4),))
    route_ids_keys = jax.random.split(jax.random.fold_in(seeds[14], 1), BATCH // SEQ_DEV)
    route_ids_turns = jax.random.permutation(jax.random.fold_in(seeds[14], 3), BATCH // SEQ_DEV)
    route_ids = jax.vmap(lambda own, number: deal_out(jax.random.fold_in(seeds[14], 2), own, number, SEQ_DEV, EXPERTS, TOPK, CAP, 2))(route_ids_keys, route_ids_turns).reshape((BATCH, TOPK))
    route_logits = noise(seeds[15], (BATCH, TOPK), 1.0, 5.0, ((0, 8),), jnp.float32)
    expert_gate = noise(seeds[16], (EXPERTS, D, FFE), D ** -0.5, 0.09375, ((0, 8), (2, 4)))
    expert_up = noise(seeds[17], (EXPERTS, D, FFE), D ** -0.5, 0.09375, ((0, 8), (2, 4)))
    expert_down = noise(seeds[18], (EXPERTS, FFE, D), FFE ** -0.5, 0.109375, ((0, 8), (1, 4)))
    dense_gate = noise(seeds[19], (D, FFD), D ** -0.5, 0.09375, ((0, 4), (1, 8)))
    dense_up = noise(seeds[20], (D, FFD), D ** -0.5, 0.09375, ((0, 4), (1, 8)))
    dense_down = noise(seeds[21], (FFD, D), FFD ** -0.5, 0.078125, ((0, 8), (1, 4)))
    branch_gate = noise(seeds[22], (D,), D ** -0.5, 0.09375)
    return dict(tokens=tokens, mix_gain=mix_gain, ffn_gain=ffn_gain, in_proj=in_proj, decay_rate=decay_rate, frequency=frequency, log_step=log_step, b_real=b_real, b_imag=b_imag, c_real=c_real, c_imag=c_imag, skip_gain=skip_gain, states=states, out_proj=out_proj, route_ids=route_ids, route_logits=route_logits, expert_gate=expert_gate, expert_up=expert_up, expert_down=expert_down, dense_gate=dense_gate, dense_up=dense_up, dense_down=dense_down, branch_gate=branch_gate)


def rms_norm(values, gain):
    flt = values.astype(jnp.float32)
    scaled = flt * lax.rsqrt(lax.optimization_barrier(jnp.mean(flt * flt, axis=-1, keepdims=True)) + 1e-06)
    return (scaled * gain.astype(jnp.float32)).astype(jnp.bfloat16)

def discretize(decay_rate, frequency, log_step, b_real, b_imag):
    step_size = jnp.exp(log_step)[:, None]
    lam_re = -decay_rate
    lam_im = frequency
    magnitude = jnp.exp(lam_re * step_size)
    abar_re = magnitude * jnp.cos(lam_im * step_size)
    abar_im = magnitude * jnp.sin(lam_im * step_size)
    denom = lam_re * lam_re + lam_im * lam_im
    fac_re = ((abar_re - 1.0) * lam_re + abar_im * lam_im) / denom
    fac_im = (abar_im * lam_re - (abar_re - 1.0) * lam_im) / denom
    bbar_re = fac_re[..., None] * b_real - fac_im[..., None] * b_imag
    bbar_im = fac_re[..., None] * b_imag + fac_im[..., None] * b_real
    return (abar_re, abar_im, bbar_re, bbar_im)

def state_step(drive, states, decay_rate, frequency, log_step, b_real, b_imag, c_real, c_imag, skip_gain):
    count = drive.shape[0]
    groups = decay_rate.shape[0]
    abar_re, abar_im, bbar_re, bbar_im = discretize(decay_rate, frequency, log_step, b_real, b_imag)
    grouped = drive.astype(jnp.float32).reshape(count, groups, GROUP)
    old_re = states[0].reshape(count, groups, STATE)
    old_im = states[1].reshape(count, groups, STATE)
    high = lax.Precision.HIGHEST
    push_re = jnp.einsum('ngh,gph->ngp', grouped, bbar_re, precision=high)
    push_im = jnp.einsum('ngh,gph->ngp', grouped, bbar_im, precision=high)
    new_re = abar_re * old_re - abar_im * old_im + push_re
    new_im = abar_re * old_im + abar_im * old_re + push_im
    readout = jnp.einsum('ngp,ghp->ngh', new_re, c_real, precision=high) - jnp.einsum('ngp,ghp->ngh', new_im, c_imag, precision=high) + skip_gain.reshape(groups, GROUP) * grouped
    reads = jax.nn.gelu(readout.reshape(count, groups * GROUP)).astype(jnp.bfloat16)
    fresh = jnp.stack([new_re.reshape(count, groups * STATE), new_im.reshape(count, groups * STATE)])
    return (reads, fresh)

def reference(tokens, mix_gain, ffn_gain, in_proj, decay_rate, frequency, log_step, b_real, b_imag, c_real, c_imag, skip_gain, states, out_proj, route_ids, route_logits, expert_gate, expert_up, expert_down, dense_gate, dense_up, dense_down, branch_gate):
    normed = rms_norm(tokens, mix_gain)
    drive = jnp.dot(normed, in_proj, preferred_element_type=jnp.float32).astype(jnp.bfloat16)
    reads, new_states = state_step(drive, states, decay_rate, frequency, log_step, b_real, b_imag, c_real, c_imag, skip_gain)
    block_width = S5W // N_TP
    mixed = jnp.zeros((BATCH, D), jnp.float32)
    for block in range(N_TP):
        piece = jnp.dot(reads[:, block * block_width:(block + 1) * block_width], out_proj[block * block_width:(block + 1) * block_width], preferred_element_type=jnp.float32).astype(jnp.bfloat16)
        mixed = mixed + piece.astype(jnp.float32)
    mixed = mixed.astype(jnp.bfloat16)
    resid = (tokens.astype(jnp.float32) + mixed.astype(jnp.float32)).astype(jnp.bfloat16)
    normed_two = rms_norm(resid, ffn_gain)
    route_weights = jax.nn.softmax(route_logits, axis=-1)
    blocked_ids = route_ids.reshape(N_EP, SEQ_DEV * TOPK)
    onehot = (blocked_ids[..., None] == jnp.arange(EXPERTS, dtype=jnp.int32)[None, None, :]).astype(jnp.int32)
    rank = jnp.cumsum(onehot, axis=1) - onehot
    slot = lax.optimization_barrier(jnp.sum(rank * onehot, axis=-1))
    block_index = jnp.arange(N_EP, dtype=jnp.int32)[:, None]
    position = blocked_ids * (N_EP * CAP) + block_index * CAP + slot
    token_index = block_index * SEQ_DEV + jnp.arange(SEQ_DEV * TOPK, dtype=jnp.int32)[None, :] // TOPK
    table = jnp.full((EXPERTS * N_EP * CAP,), BATCH, jnp.int32).at[position.reshape(-1)].set(token_index.reshape(-1))
    padded = jnp.concatenate([normed_two, jnp.zeros((1, D), jnp.bfloat16)], axis=0)
    hidden_block = FFE // N_TP

    def one_expert(inputs):
        index_row, gate_w, up_w, down_w = inputs
        rows_in = padded[index_row]
        summed = jnp.zeros((N_EP * CAP, D), jnp.float32)
        for block in range(N_TP):
            lo = block * hidden_block
            gate_val = jnp.dot(rows_in, gate_w[:, lo:lo + hidden_block], preferred_element_type=jnp.float32)
            up_val = jnp.dot(rows_in, up_w[:, lo:lo + hidden_block], preferred_element_type=jnp.float32)
            hidden = (jax.nn.silu(gate_val) * up_val).astype(jnp.bfloat16)
            piece = jnp.dot(hidden, down_w[lo:lo + hidden_block], preferred_element_type=jnp.float32)
            summed = summed + piece.astype(jnp.bfloat16).astype(jnp.float32)
        return summed.astype(jnp.bfloat16)
    expert_out = lax.map(one_expert, (table.reshape(EXPERTS, N_EP * CAP), expert_gate, expert_up, expert_down))
    picked = expert_out.reshape(EXPERTS * N_EP * CAP, D)[position.reshape(-1)]
    picked = picked.reshape(BATCH, TOPK, D).astype(jnp.float32)
    routed = lax.optimization_barrier(jnp.sum(route_weights[..., None] * picked, axis=1))
    gate_val = jnp.dot(normed_two, dense_gate, preferred_element_type=jnp.float32)
    up_val = jnp.dot(normed_two, dense_up, preferred_element_type=jnp.float32)
    dense_hidden = (jax.nn.silu(gate_val) * up_val).astype(jnp.bfloat16)
    dense_term = jnp.dot(dense_hidden, dense_down, preferred_element_type=jnp.float32)
    branch = jax.nn.sigmoid(jnp.dot(normed_two, branch_gate, preferred_element_type=jnp.float32))
    output = (resid.astype(jnp.float32) + routed + branch[:, None] * dense_term).astype(jnp.bfloat16)
    return (output, new_states)
```

```python
import functools
import jax
import jax.numpy as jnp
from jax import lax
from jax.experimental import pallas as pl
from jax.experimental.pallas import tpu as pltpu
from jax.sharding import PartitionSpec as P

GROUP = 16
STATE = 64
MESH = pl.DeviceIdType.MESH


def fast_extent(axis, size):
    if axis == "tp":
        return 2
    extent = 1
    while (2 * extent) * (2 * extent) * 2 <= size:
        extent *= 2
    return extent


class Grid:
    def __init__(self, axis, size):
        self.axis, self.size = axis, size
        self.fast = fast_extent(axis, size)
        self.slow = size // self.fast
        self.me = lax.axis_index(axis)
        self.at_fast = self.me % self.fast
        self.at_slow = self.me // self.fast

    def index(self, slow_step, fast_step):
        slow_at = (self.at_slow + slow_step + self.slow) % self.slow
        fast_at = (self.at_fast + fast_step + self.fast) % self.fast
        return slow_at * self.fast + fast_at

    def peers(self):
        return [self.index(k, 0) for k in range(1, self.slow)] + [
            self.index(0, q) for q in range(1, self.fast)
        ]

    def greet(self):
        barrier = pltpu.get_barrier_semaphore()
        peers = self.peers()
        for peer in peers:
            pl.semaphore_signal(barrier, inc=1, device_id={self.axis: peer}, device_id_type=MESH)
        pl.semaphore_wait(barrier, len(peers))

    def copy(self, source, target, sent, landed, peer):
        return pltpu.make_async_remote_copy(
            src_ref=source,
            dst_ref=target,
            send_sem=sent,
            recv_sem=landed,
            device_id={self.axis: peer},
            device_id_type=MESH,
        )


def part_of(ref, owner, start, rows, width, cols):
    if cols:
        return ref.at[pl.ds(start, rows), pl.ds(pl.multiple_of(owner * width, 128), width)]
    return ref.at[owner, pl.ds(start, rows), :]


def gather_kernel(axis, size, pieces, cols, *refs):
    count = len(pieces)
    ins, outs = refs[:count], refs[count : 2 * count]
    slow_sent, slow_landed, fast_sent, fast_landed, own_sem = refs[2 * count :]
    grid = Grid(axis, size)
    spans = []
    for item, number in enumerate(pieces):
        rows = ins[item].shape[0] // number
        spans += [(item, j, j * rows, rows) for j in range(number)]

    def place(item, owner, start, rows):
        return part_of(outs[item], owner, start, rows, ins[item].shape[1], cols)

    grid.greet()
    pending = []
    for item, j, start, rows in spans:
        for k in range(1, grid.slow):
            copy = grid.copy(
                ins[item].at[pl.ds(start, rows), :],
                place(item, grid.me, start, rows),
                slow_sent.at[item, j, k - 1],
                slow_landed.at[item, j, k - 1],
                grid.index(k, 0),
            )
            copy.start()
            pending.append(copy)
    for item, j, start, rows in spans:
        for q in range(1, grid.fast):
            copy = grid.copy(
                ins[item].at[pl.ds(start, rows), :],
                place(item, grid.me, start, rows),
                fast_sent.at[item, j, 0, q - 1],
                fast_landed.at[item, j, 0, q - 1],
                grid.index(0, q),
            )
            copy.start()
            pending.append(copy)
    owns = []
    for item in range(count):
        own = pltpu.make_async_copy(
            ins[item], place(item, grid.me, 0, ins[item].shape[0]), own_sem.at[item]
        )
        own.start()
        owns.append(own)
    for item, j, start, rows in spans:
        for k in range(1, grid.slow):
            block = place(item, grid.index(-k, 0), start, rows)
            grid.copy(
                block,
                block,
                slow_sent.at[item, j, k - 1],
                slow_landed.at[item, j, k - 1],
                grid.index(-k, 0),
            ).wait_recv()
            for q in range(1, grid.fast):
                copy = grid.copy(
                    block,
                    block,
                    fast_sent.at[item, j, k, q - 1],
                    fast_landed.at[item, j, k, q - 1],
                    grid.index(0, q),
                )
                copy.start()
                pending.append(copy)
    for item, j, start, rows in spans:
        for k in range(grid.slow):
            for q in range(1, grid.fast):
                block = place(item, grid.index(-k, -q), start, rows)
                grid.copy(
                    block,
                    block,
                    fast_sent.at[item, j, k, q - 1],
                    fast_landed.at[item, j, k, q - 1],
                    grid.index(0, -q),
                ).wait_recv()
    for copy in pending:
        copy.wait_send()
    for own in owns:
        own.wait()


def all_gather(arrays, axis, size, pieces, cols, collective_id):
    shapes = []
    for array in arrays:
        rows, width = array.shape
        shape = (rows, size * width) if cols else (size, rows, width)
        shapes.append(jax.ShapeDtypeStruct(shape, array.dtype))
    fast = fast_extent(axis, size)
    slow = size // fast
    count, most = len(arrays), max(pieces)
    sems = [
        pltpu.SemaphoreType.DMA((count, most, slow - 1)),
        pltpu.SemaphoreType.DMA((count, most, slow - 1)),
        pltpu.SemaphoreType.DMA((count, most, slow, fast - 1)),
        pltpu.SemaphoreType.DMA((count, most, slow, fast - 1)),
        pltpu.SemaphoreType.DMA((count,)),
    ]
    return pl.pallas_call(
        functools.partial(gather_kernel, axis, size, pieces, cols),
        out_shape=shapes,
        in_specs=[pl.BlockSpec(memory_space=pltpu.VMEM)] * count,
        out_specs=[pl.BlockSpec(memory_space=pltpu.VMEM)] * count,
        scratch_shapes=sems,
        compiler_params=pltpu.CompilerParams(
            collective_id=collective_id, has_side_effects=True, vmem_limit_bytes=16 << 20
        ),
    )(*arrays)


def reduce_kernel(
    axis,
    size,
    number,
    cols,
    x_ref,
    o_ref,
    got_fast,
    mid,
    got_slow,
    total_ref,
    fast_sent,
    fast_landed,
    slow_sent,
    slow_landed,
):
    grid = Grid(axis, size)
    rows, width = o_ref.shape
    step = rows // number
    grid.greet()
    pending = []
    for k in range(1, grid.slow + 1):
        for j in range(number):
            for q in range(1, grid.fast):
                copy = grid.copy(
                    part_of(x_ref, grid.index(k, q), j * step, step, width, cols),
                    got_fast.at[q - 1, k - 1, pl.ds(j * step, step), :],
                    fast_sent.at[q - 1, k - 1, j],
                    fast_landed.at[q - 1, k - 1, j],
                    grid.index(0, q),
                )
                copy.start()
                pending.append(copy)
    for k in range(1, grid.slow + 1):
        for j in range(number):
            span = pl.ds(j * step, step)
            total = part_of(x_ref, grid.index(k, 0), j * step, step, width, cols)[...].astype(
                jnp.float32
            )
            for q in range(1, grid.fast):
                block = got_fast.at[q - 1, k - 1, span, :]
                grid.copy(
                    block,
                    block,
                    fast_sent.at[q - 1, k - 1, j],
                    fast_landed.at[q - 1, k - 1, j],
                    grid.index(0, -q),
                ).wait_recv()
                total = total + block[...].astype(jnp.float32)
            if k == grid.slow:
                total_ref[span, :] = total
            else:
                mid[k - 1, span, :] = total.astype(mid.dtype)
                copy = grid.copy(
                    mid.at[k - 1, span, :],
                    got_slow.at[k - 1, span, :],
                    slow_sent.at[k - 1, j],
                    slow_landed.at[k - 1, j],
                    grid.index(k, 0),
                )
                copy.start()
                pending.append(copy)
    for j in range(number):
        span = pl.ds(j * step, step)
        total = total_ref[span, :]
        for k in range(1, grid.slow):
            block = got_slow.at[k - 1, span, :]
            grid.copy(
                block,
                block,
                slow_sent.at[k - 1, j],
                slow_landed.at[k - 1, j],
                grid.index(-k, 0),
            ).wait_recv()
            total = total + block[...].astype(jnp.float32)
        o_ref[span, :] = total.astype(o_ref.dtype)
    for copy in pending:
        copy.wait_send()


def reduce_scatter(array, axis, size, number, cols, collective_id):
    if cols:
        rows, width = array.shape[0], array.shape[1] // size
    else:
        rows, width = array.shape[1:]
    fast = fast_extent(axis, size)
    slow = size // fast
    return pl.pallas_call(
        functools.partial(reduce_kernel, axis, size, number, cols),
        out_shape=jax.ShapeDtypeStruct((rows, width), array.dtype),
        in_specs=[pl.BlockSpec(memory_space=pltpu.VMEM)],
        out_specs=pl.BlockSpec(memory_space=pltpu.VMEM),
        scratch_shapes=[
            pltpu.VMEM((fast - 1, slow, rows, width), array.dtype),
            pltpu.VMEM((slow - 1, rows, width), array.dtype),
            pltpu.VMEM((slow - 1, rows, width), array.dtype),
            pltpu.VMEM((rows, width), jnp.float32),
            pltpu.SemaphoreType.DMA((fast - 1, slow, number)),
            pltpu.SemaphoreType.DMA((fast - 1, slow, number)),
            pltpu.SemaphoreType.DMA((slow - 1, number)),
            pltpu.SemaphoreType.DMA((slow - 1, number)),
        ],
        compiler_params=pltpu.CompilerParams(
            collective_id=collective_id, has_side_effects=True, vmem_limit_bytes=24 << 20
        ),
    )(array)

def rms_norm(values, gain):
    flt = values.astype(jnp.float32)
    scaled = flt * lax.rsqrt(jnp.mean(flt * flt, axis=-1, keepdims=True) + 1e-06)
    return (scaled * gain).astype(jnp.bfloat16)


def discretize(decay_rate, frequency, log_step, b_real, b_imag):
    step_size = jnp.exp(log_step)[:, None]
    lam_re = -decay_rate
    magnitude = jnp.exp(lam_re * step_size)
    abar_re = magnitude * jnp.cos(frequency * step_size)
    abar_im = magnitude * jnp.sin(frequency * step_size)
    denom = lam_re * lam_re + frequency * frequency
    fac_re = ((abar_re - 1.0) * lam_re + abar_im * frequency) / denom
    fac_im = (abar_im * lam_re - (abar_re - 1.0) * frequency) / denom
    bbar_re = fac_re[..., None] * b_real - fac_im[..., None] * b_imag
    bbar_im = fac_re[..., None] * b_imag + fac_im[..., None] * b_real
    return (abar_re, abar_im, bbar_re, bbar_im)


def state_step(
    drive, states, decay_rate, frequency, log_step, b_real, b_imag, c_real, c_imag, skip_gain
):
    count = drive.shape[0]
    groups = decay_rate.shape[0]
    abar_re, abar_im, bbar_re, bbar_im = discretize(decay_rate, frequency, log_step, b_real, b_imag)
    grouped = drive.astype(jnp.float32).reshape(count, groups, GROUP)
    old_re = states[0].reshape(count, groups, STATE)
    old_im = states[1].reshape(count, groups, STATE)
    high = lax.Precision.HIGHEST
    push_re = jnp.einsum("ngh,gph->ngp", grouped, bbar_re, precision=high)
    push_im = jnp.einsum("ngh,gph->ngp", grouped, bbar_im, precision=high)
    new_re = abar_re * old_re - abar_im * old_im + push_re
    new_im = abar_re * old_im + abar_im * old_re + push_im
    readout = (
        jnp.einsum("ngp,ghp->ngh", new_re, c_real, precision=high)
        - jnp.einsum("ngp,ghp->ngh", new_im, c_imag, precision=high)
        + skip_gain.reshape(groups, GROUP) * grouped
    )
    reads = jax.nn.gelu(readout.reshape(count, groups * GROUP)).astype(jnp.bfloat16)
    fresh = jnp.stack(
        [new_re.reshape(count, groups * STATE), new_im.reshape(count, groups * STATE)]
    )
    return (reads, fresh)


def shards(
    tokens,
    mix_gain,
    ffn_gain,
    in_proj,
    decay_rate,
    frequency,
    log_step,
    b_real,
    b_imag,
    c_real,
    c_imag,
    skip_gain,
    states,
    out_proj,
    route_ids,
    route_logits,
    expert_gate,
    expert_up,
    expert_down,
    dense_gate,
    dense_up,
    dense_down,
    branch_gate,
):
    seq_count, width = tokens.shape
    tp_count = lax.axis_size("tp")
    ep_count = lax.axis_size("ep")
    tp_index = lax.axis_index("tp")
    part_width = width // tp_count
    normed = rms_norm(tokens, mix_gain)
    drive = jnp.dot(normed, in_proj, preferred_element_type=jnp.float32).astype(jnp.bfloat16)
    reads, new_states = state_step(
        drive, states, decay_rate, frequency, log_step, b_real, b_imag, c_real, c_imag, skip_gain
    )
    partial_value = (
        jnp.dot(reads, out_proj, preferred_element_type=jnp.float32)
        .astype(jnp.bfloat16)
        .astype(jnp.float32)
    )
    mixed_cols = reduce_scatter(partial_value.astype(jnp.bfloat16), "tp", tp_count, 2, True, 0)
    (mixed,) = all_gather([mixed_cols], "tp", tp_count, [2], True, 1)
    resid = (tokens.astype(jnp.float32) + mixed.astype(jnp.float32)).astype(jnp.bfloat16)
    normed_two = rms_norm(resid, ffn_gain)
    own_cols = lax.dynamic_slice_in_dim(normed_two, tp_index * part_width, part_width, 1)
    branch = jax.nn.sigmoid(jnp.dot(normed_two, branch_gate, preferred_element_type=jnp.float32))
    route_weights = jax.nn.softmax(route_logits, axis=-1)
    top_count = route_ids.shape[1]
    side = jnp.concatenate(
        [route_ids.astype(jnp.float32), route_weights, branch[:, None]], axis=1
    )
    side = jnp.pad(side, ((0, 0), (0, 128 - side.shape[1])))
    every_cols, every_side = all_gather([own_cols, side], "ep", ep_count, [1, 1], False, 2)
    total_count = ep_count * seq_count
    every_cols = every_cols.reshape(total_count, part_width)
    every_side = every_side.reshape(total_count, 128)
    every_ids = every_side[:, :top_count]
    every_weights = every_side[:, top_count : 2 * top_count]
    every_branch = every_side[:, 2 * top_count]
    mine = every_ids == lax.axis_index("ep").astype(jnp.float32)
    taken = jnp.any(mine, axis=1)
    own_weight = jnp.sum(jnp.where(mine, every_weights, 0.0), axis=1)
    order = jnp.cumsum(taken.astype(jnp.int32)) - 1
    room = ep_count * max(2, 2 * seq_count * top_count // ep_count)
    slots = jnp.arange(room, dtype=jnp.int32)
    select = (order[None, :] == slots[:, None]) & taken[None, :]
    row_weight = jnp.sum(jnp.where(select, own_weight[None, :], 0.0), axis=1)
    select = select.astype(jnp.bfloat16)
    expert_in = jnp.dot(select, every_cols, preferred_element_type=jnp.float32).astype(jnp.bfloat16)
    (full_rows,) = all_gather([expert_in], "tp", tp_count, [4], True, 3)
    hidden_width = dense_gate.shape[1]
    gate_part = jnp.dot(every_cols, dense_gate, preferred_element_type=jnp.float32)
    up_part = jnp.dot(every_cols, dense_up, preferred_element_type=jnp.float32)
    both = jnp.concatenate([gate_part.astype(jnp.bfloat16), up_part.astype(jnp.bfloat16)], axis=1)
    both = both.reshape(tp_count, total_count // tp_count, 2 * hidden_width)
    summed = reduce_scatter(both, "tp", tp_count, 4, False, 4).astype(jnp.float32)
    own_hidden = (
        jax.nn.silu(summed[:, :hidden_width]) * summed[:, hidden_width:]
    ).astype(jnp.bfloat16)
    (dense_hidden,) = all_gather([own_hidden], "tp", tp_count, [2], False, 5)
    dense_hidden = dense_hidden.reshape(total_count, hidden_width)
    gate_val = jnp.dot(full_rows, expert_gate[0], preferred_element_type=jnp.float32)
    up_val = jnp.dot(full_rows, expert_up[0], preferred_element_type=jnp.float32)
    hidden = (jax.nn.silu(gate_val) * up_val).astype(jnp.bfloat16)
    expert_part = jnp.dot(hidden, expert_down[0], preferred_element_type=jnp.float32)
    expert_cols = reduce_scatter(expert_part.astype(jnp.bfloat16), "tp", tp_count, 4, True, 6)
    weighted = (expert_cols.astype(jnp.float32) * row_weight[:, None]).astype(jnp.bfloat16)
    routed_part = lax.dot_general(
        select, weighted, (((0,), (0,)), ((), ())), preferred_element_type=jnp.float32
    )
    dense_part = jnp.dot(dense_hidden, dense_down, preferred_element_type=jnp.float32)
    share = (routed_part + every_branch[:, None] * dense_part).astype(jnp.bfloat16)
    share = share.reshape(ep_count, seq_count, part_width)
    gathered = reduce_scatter(share, "ep", ep_count, 1, False, 7)
    resid_cols = lax.dynamic_slice_in_dim(resid, tp_index * part_width, part_width, 1)
    output = (resid_cols.astype(jnp.float32) + gathered.astype(jnp.float32)).astype(jnp.bfloat16)
    return (output, new_states)


def solution(mesh):
    return jax.shard_map(
        shards,
        mesh=mesh,
        in_specs=(
            P("ep", None),
            P(),
            P(),
            P(None, "tp"),
            P("tp", None),
            P("tp", None),
            P("tp"),
            P("tp", None, None),
            P("tp", None, None),
            P("tp", None, None),
            P("tp", None, None),
            P("tp"),
            P(None, "ep", "tp"),
            P("tp", None),
            P("ep", None),
            P("ep", None),
            P("ep", None, "tp"),
            P("ep", None, "tp"),
            P("ep", "tp", None),
            P("tp", "ep"),
            P("tp", "ep"),
            P("ep", "tp"),
            P(),
        ),
        out_specs=(P("ep", "tp"), P(None, "ep", "tp")),
        check_vma=False,
    )
```

```python
import functools
import jax
import jax.numpy as jnp
from jax import lax
from jax.experimental import pallas as pl
from jax.experimental.pallas import tpu as pltpu
from jax.sharding import PartitionSpec as P

GROUP = 16
STATE = 64
MESH = pl.DeviceIdType.MESH


def fast_extent(axis, size):
    if axis == "tp":
        return 2
    extent = 1
    while (2 * extent) * (2 * extent) * 2 <= size:
        extent *= 2
    return extent


class Grid:
    def __init__(self, axis, size):
        self.axis, self.size = axis, size
        self.fast = fast_extent(axis, size)
        self.slow = size // self.fast
        self.me = lax.axis_index(axis)
        self.at_fast = self.me % self.fast
        self.at_slow = self.me // self.fast

    def index(self, slow_step, fast_step):
        slow_at = (self.at_slow + slow_step + self.slow) % self.slow
        fast_at = (self.at_fast + fast_step + self.fast) % self.fast
        return slow_at * self.fast + fast_at

    def peers(self):
        return [self.index(k, 0) for k in range(1, self.slow)] + [
            self.index(0, q) for q in range(1, self.fast)
        ]

    def greet(self):
        barrier = pltpu.get_barrier_semaphore()
        peers = self.peers()
        for peer in peers:
            pl.semaphore_signal(barrier, inc=1, device_id={self.axis: peer}, device_id_type=MESH)
        pl.semaphore_wait(barrier, len(peers))

    def copy(self, source, target, sent, landed, peer):
        return pltpu.make_async_remote_copy(
            src_ref=source,
            dst_ref=target,
            send_sem=sent,
            recv_sem=landed,
            device_id={self.axis: peer},
            device_id_type=MESH,
        )


def part_of(ref, owner, start, rows, width, cols):
    if cols:
        return ref.at[pl.ds(start, rows), pl.ds(pl.multiple_of(owner * width, 128), width)]
    return ref.at[owner, pl.ds(start, rows), :]


def gather_kernel(axis, size, pieces, cols, *refs):
    count = len(pieces)
    ins, outs = refs[:count], refs[count : 2 * count]
    slow_sent, slow_landed, fast_sent, fast_landed, own_sem = refs[2 * count :]
    grid = Grid(axis, size)
    spans = []
    for item, number in enumerate(pieces):
        rows = ins[item].shape[0] // number
        spans += [(item, j, j * rows, rows) for j in range(number)]

    def place(item, owner, start, rows):
        return part_of(outs[item], owner, start, rows, ins[item].shape[1], cols)

    grid.greet()
    pending = []
    for item, j, start, rows in spans:
        for k in range(1, grid.slow):
            copy = grid.copy(
                ins[item].at[pl.ds(start, rows), :],
                place(item, grid.me, start, rows),
                slow_sent.at[item, j, k - 1],
                slow_landed.at[item, j, k - 1],
                grid.index(k, 0),
            )
            copy.start()
            pending.append(copy)
    for item, j, start, rows in spans:
        for q in range(1, grid.fast):
            copy = grid.copy(
                ins[item].at[pl.ds(start, rows), :],
                place(item, grid.me, start, rows),
                fast_sent.at[item, j, 0, q - 1],
                fast_landed.at[item, j, 0, q - 1],
                grid.index(0, q),
            )
            copy.start()
            pending.append(copy)
    owns = []
    for item in range(count):
        own = pltpu.make_async_copy(
            ins[item], place(item, grid.me, 0, ins[item].shape[0]), own_sem.at[item]
        )
        own.start()
        owns.append(own)
    for item, j, start, rows in spans:
        for k in range(1, grid.slow):
            block = place(item, grid.index(-k, 0), start, rows)
            grid.copy(
                block,
                block,
                slow_sent.at[item, j, k - 1],
                slow_landed.at[item, j, k - 1],
                grid.index(-k, 0),
            ).wait_recv()
            for q in range(1, grid.fast):
                copy = grid.copy(
                    block,
                    block,
                    fast_sent.at[item, j, k, q - 1],
                    fast_landed.at[item, j, k, q - 1],
                    grid.index(0, q),
                )
                copy.start()
                pending.append(copy)
    for item, j, start, rows in spans:
        for k in range(grid.slow):
            for q in range(1, grid.fast):
                block = place(item, grid.index(-k, -q), start, rows)
                grid.copy(
                    block,
                    block,
                    fast_sent.at[item, j, k, q - 1],
                    fast_landed.at[item, j, k, q - 1],
                    grid.index(0, -q),
                ).wait_recv()
    for copy in pending:
        copy.wait_send()
    for own in owns:
        own.wait()


def all_gather(arrays, axis, size, pieces, cols, collective_id):
    shapes = []
    for array in arrays:
        rows, width = array.shape
        shape = (rows, size * width) if cols else (size, rows, width)
        shapes.append(jax.ShapeDtypeStruct(shape, array.dtype))
    fast = fast_extent(axis, size)
    slow = size // fast
    count, most = len(arrays), max(pieces)
    sems = [
        pltpu.SemaphoreType.DMA((count, most, slow - 1)),
        pltpu.SemaphoreType.DMA((count, most, slow - 1)),
        pltpu.SemaphoreType.DMA((count, most, slow, fast - 1)),
        pltpu.SemaphoreType.DMA((count, most, slow, fast - 1)),
        pltpu.SemaphoreType.DMA((count,)),
    ]
    return pl.pallas_call(
        functools.partial(gather_kernel, axis, size, pieces, cols),
        out_shape=shapes,
        in_specs=[pl.BlockSpec(memory_space=pltpu.VMEM)] * count,
        out_specs=[pl.BlockSpec(memory_space=pltpu.VMEM)] * count,
        scratch_shapes=sems,
        compiler_params=pltpu.CompilerParams(
            collective_id=collective_id, has_side_effects=True, vmem_limit_bytes=16 << 20
        ),
    )(*arrays)


def reduce_kernel(
    axis,
    size,
    number,
    cols,
    x_ref,
    o_ref,
    got_fast,
    mid,
    got_slow,
    total_ref,
    fast_sent,
    fast_landed,
    slow_sent,
    slow_landed,
):
    grid = Grid(axis, size)
    rows, width = o_ref.shape
    step = rows // number
    grid.greet()
    pending = []
    for k in range(1, grid.slow + 1):
        for j in range(number):
            for q in range(1, grid.fast):
                copy = grid.copy(
                    part_of(x_ref, grid.index(k, q), j * step, step, width, cols),
                    got_fast.at[q - 1, k - 1, pl.ds(j * step, step), :],
                    fast_sent.at[q - 1, k - 1, j],
                    fast_landed.at[q - 1, k - 1, j],
                    grid.index(0, q),
                )
                copy.start()
                pending.append(copy)
    for k in range(1, grid.slow + 1):
        for j in range(number):
            span = pl.ds(j * step, step)
            total = part_of(x_ref, grid.index(k, 0), j * step, step, width, cols)[...].astype(
                jnp.float32
            )
            for q in range(1, grid.fast):
                block = got_fast.at[q - 1, k - 1, span, :]
                grid.copy(
                    block,
                    block,
                    fast_sent.at[q - 1, k - 1, j],
                    fast_landed.at[q - 1, k - 1, j],
                    grid.index(0, -q),
                ).wait_recv()
                total = total + block[...].astype(jnp.float32)
            if k == grid.slow:
                total_ref[span, :] = total
            else:
                mid[k - 1, span, :] = total.astype(mid.dtype)
                copy = grid.copy(
                    mid.at[k - 1, span, :],
                    got_slow.at[k - 1, span, :],
                    slow_sent.at[k - 1, j],
                    slow_landed.at[k - 1, j],
                    grid.index(k, 0),
                )
                copy.start()
                pending.append(copy)
    for j in range(number):
        span = pl.ds(j * step, step)
        total = total_ref[span, :]
        for k in range(1, grid.slow):
            block = got_slow.at[k - 1, span, :]
            grid.copy(
                block,
                block,
                slow_sent.at[k - 1, j],
                slow_landed.at[k - 1, j],
                grid.index(-k, 0),
            ).wait_recv()
            total = total + block[...].astype(jnp.float32)
        o_ref[span, :] = total.astype(o_ref.dtype)
    for copy in pending:
        copy.wait_send()


def reduce_scatter(array, axis, size, number, cols, collective_id):
    if cols:
        rows, width = array.shape[0], array.shape[1] // size
    else:
        rows, width = array.shape[1:]
    fast = fast_extent(axis, size)
    slow = size // fast
    return pl.pallas_call(
        functools.partial(reduce_kernel, axis, size, number, cols),
        out_shape=jax.ShapeDtypeStruct((rows, width), array.dtype),
        in_specs=[pl.BlockSpec(memory_space=pltpu.VMEM)],
        out_specs=pl.BlockSpec(memory_space=pltpu.VMEM),
        scratch_shapes=[
            pltpu.VMEM((fast - 1, slow, rows, width), array.dtype),
            pltpu.VMEM((slow - 1, rows, width), array.dtype),
            pltpu.VMEM((slow - 1, rows, width), array.dtype),
            pltpu.VMEM((rows, width), jnp.float32),
            pltpu.SemaphoreType.DMA((fast - 1, slow, number)),
            pltpu.SemaphoreType.DMA((fast - 1, slow, number)),
            pltpu.SemaphoreType.DMA((slow - 1, number)),
            pltpu.SemaphoreType.DMA((slow - 1, number)),
        ],
        compiler_params=pltpu.CompilerParams(
            collective_id=collective_id, has_side_effects=True, vmem_limit_bytes=24 << 20
        ),
    )(array)

class Gather:
    def __init__(self, grid, source, target, number, cols, sems):
        self.grid, self.source, self.target, self.cols = grid, source, target, cols
        self.slow_sent, self.slow_landed, self.fast_sent, self.fast_landed, self.own_sem = sems
        self.rows, self.width = source.shape
        self.step = self.rows // number
        self.number = number
        self.pending = []

    def place(self, owner, j):
        return part_of(self.target, owner, j * self.step, self.step, self.width, self.cols)

    def slow_copy(self, source, target, j, k, peer):
        return self.grid.copy(
            source, target, self.slow_sent.at[j, k - 1], self.slow_landed.at[j, k - 1], peer
        )

    def fast_copy(self, source, target, j, k, q, peer):
        return self.grid.copy(
            source, target, self.fast_sent.at[j, k, q - 1], self.fast_landed.at[j, k, q - 1], peer
        )

    def launch(self, copy):
        copy.start()
        self.pending.append(copy)

    def start(self):
        grid = self.grid
        for j in range(self.number):
            piece = self.source.at[pl.ds(j * self.step, self.step), :]
            spot = self.place(grid.me, j)
            for k in range(1, grid.slow):
                self.launch(self.slow_copy(piece, spot, j, k, grid.index(k, 0)))
        for j in range(self.number):
            piece = self.source.at[pl.ds(j * self.step, self.step), :]
            spot = self.place(grid.me, j)
            for q in range(1, grid.fast):
                self.launch(self.fast_copy(piece, spot, j, 0, q, grid.index(0, q)))
        self.own = pltpu.make_async_copy(
            self.source,
            part_of(self.target, grid.me, 0, self.rows, self.width, self.cols),
            self.own_sem,
        )
        self.own.start()

    def relay(self):
        grid = self.grid
        for j in range(self.number):
            for k in range(1, grid.slow):
                spot = self.place(grid.index(-k, 0), j)
                self.slow_copy(spot, spot, j, k, grid.index(-k, 0)).wait_recv()
                for q in range(1, grid.fast):
                    self.launch(self.fast_copy(spot, spot, j, k, q, grid.index(0, q)))

    def arrive(self):
        grid = self.grid
        for j in range(self.number):
            for k in range(grid.slow):
                for q in range(1, grid.fast):
                    spot = self.place(grid.index(-k, -q), j)
                    self.fast_copy(spot, spot, j, k, q, grid.index(0, -q)).wait_recv()
        self.own.wait()

    def finish(self):
        for copy in self.pending:
            copy.wait_send()


def gather_sems(grid_fast, grid_slow, number):
    return [
        pltpu.SemaphoreType.DMA((number, grid_slow - 1)),
        pltpu.SemaphoreType.DMA((number, grid_slow - 1)),
        pltpu.SemaphoreType.DMA((number, grid_slow, grid_fast - 1)),
        pltpu.SemaphoreType.DMA((number, grid_slow, grid_fast - 1)),
        pltpu.SemaphoreType.DMA,
    ]


class Reduce:
    def __init__(self, grid, source, number, cols, scratch):
        self.grid, self.source, self.cols, self.number = grid, source, cols, number
        self.got_fast, self.mid, self.got_slow, self.total = scratch[:4]
        self.fast_sent, self.fast_landed, self.slow_sent, self.slow_landed = scratch[4:]
        rows, self.width = self.total.shape
        self.step = rows // number
        self.pending = []

    def part(self, dest, j):
        return part_of(self.source, dest, j * self.step, self.step, self.width, self.cols)

    def span(self, j):
        return pl.ds(j * self.step, self.step)

    def fast_copy(self, source, k, j, q, peer):
        return self.grid.copy(
            source,
            self.got_fast.at[q - 1, k - 1, self.span(j), :],
            self.fast_sent.at[q - 1, k - 1, j],
            self.fast_landed.at[q - 1, k - 1, j],
            peer,
        )

    def slow_copy(self, k, j, peer):
        return self.grid.copy(
            self.mid.at[k - 1, self.span(j), :],
            self.got_slow.at[k - 1, self.span(j), :],
            self.slow_sent.at[k - 1, j],
            self.slow_landed.at[k - 1, j],
            peer,
        )

    def push(self):
        grid = self.grid
        for k in range(1, grid.slow + 1):
            for j in range(self.number):
                for q in range(1, grid.fast):
                    copy = self.fast_copy(
                        self.part(grid.index(k, q), j), k, j, q, grid.index(0, q)
                    )
                    copy.start()
                    self.pending.append(copy)

    def relay(self):
        grid = self.grid
        for k in range(1, grid.slow + 1):
            for j in range(self.number):
                value = self.part(grid.index(k, 0), j)[...].astype(jnp.float32)
                for q in range(1, grid.fast):
                    block = self.got_fast.at[q - 1, k - 1, self.span(j), :]
                    self.fast_copy(block, k, j, q, grid.index(0, -q)).wait_recv()
                    value = value + block[...].astype(jnp.float32)
                if k == grid.slow:
                    self.total[self.span(j), :] = value
                else:
                    self.mid[k - 1, self.span(j), :] = value.astype(self.mid.dtype)
                    copy = self.slow_copy(k, j, grid.index(k, 0))
                    copy.start()
                    self.pending.append(copy)

    def collect(self, emit):
        grid = self.grid
        for j in range(self.number):
            value = self.total[self.span(j), :]
            for k in range(1, grid.slow):
                self.slow_copy(k, j, grid.index(-k, 0)).wait_recv()
                value = value + self.got_slow[k - 1, self.span(j), :].astype(jnp.float32)
            emit(self.span(j), value)

    def finish(self):
        for copy in self.pending:
            copy.wait_send()


def reduce_scratch(fast, slow, rows, width, number):
    return [
        pltpu.VMEM((fast - 1, slow, rows, width), jnp.bfloat16),
        pltpu.VMEM((slow - 1, rows, width), jnp.bfloat16),
        pltpu.VMEM((slow - 1, rows, width), jnp.bfloat16),
        pltpu.VMEM((rows, width), jnp.float32),
        pltpu.SemaphoreType.DMA((fast - 1, slow, number)),
        pltpu.SemaphoreType.DMA((fast - 1, slow, number)),
        pltpu.SemaphoreType.DMA((slow - 1, number)),
        pltpu.SemaphoreType.DMA((slow - 1, number)),
    ]


def tile_of(extent):
    for tile in (256, 128):
        if extent % tile == 0:
            return tile
    return extent


def branches_kernel(
    axis,
    size,
    rows_ref,
    cols_ref,
    dense_gate,
    dense_up,
    gate_hbm,
    up_hbm,
    down_hbm,
    dense_out,
    expert_out,
    full,
    gate,
    up,
    down,
    both,
    own_hidden,
    hidden,
    part,
    weight_sems,
    *rest,
):
    grid = Grid(axis, size)
    rows_gather = Gather(grid, rows_ref, full, ROW_PIECES, True, rest[:5])
    hidden_gather = Gather(grid, own_hidden, dense_out, 2, False, rest[5:10])
    dense_sum = Reduce(grid, both, 4, False, rest[10:18])
    expert_sum = Reduce(grid, part, 4, True, rest[18:26])
    loads = []
    for item, (source, target) in enumerate(((gate_hbm, gate), (up_hbm, up), (down_hbm, down))):
        load = pltpu.make_async_copy(source, target, weight_sems.at[item])
        load.start()
        loads.append(load)
    grid.greet()
    rows_gather.start()
    share, double = both.shape[1:]
    width = double // 2

    @pl.loop(0, size)
    def _(dest):
        start = pl.multiple_of(dest * share, 16)
        block = cols_ref[pl.ds(start, share), :]
        both[dest, :, :width] = jnp.dot(
            block, dense_gate[...], preferred_element_type=jnp.float32
        ).astype(jnp.bfloat16)
        both[dest, :, width:] = jnp.dot(
            block, dense_up[...], preferred_element_type=jnp.float32
        ).astype(jnp.bfloat16)

    dense_sum.push()
    dense_sum.relay()
    rows_gather.relay()
    rows_gather.arrive()
    loads[0].wait()
    loads[1].wait()
    inner = hidden.shape[1]
    tile = tile_of(inner)

    @pl.loop(0, inner // tile)
    def _(step):
        span = pl.ds(pl.multiple_of(step * tile, 128), tile)
        gate_val = jnp.dot(full[...], gate[:, span], preferred_element_type=jnp.float32)
        up_val = jnp.dot(full[...], up[:, span], preferred_element_type=jnp.float32)
        hidden[:, span] = (jax.nn.silu(gate_val) * up_val).astype(jnp.bfloat16)

    def emit_hidden(span, value):
        own_hidden[span, :] = (jax.nn.silu(value[:, :width]) * value[:, width:]).astype(
            jnp.bfloat16
        )

    dense_sum.collect(emit_hidden)
    loads[2].wait()
    hidden_gather.start()
    wide = 2 * tile_of(part.shape[1])

    @pl.loop(0, part.shape[1] // wide)
    def _(step):
        span = pl.ds(pl.multiple_of(step * wide, 128), wide)
        part[:, span] = jnp.dot(
            hidden[...], down[:, span], preferred_element_type=jnp.float32
        ).astype(jnp.bfloat16)

    expert_sum.push()
    expert_sum.relay()
    hidden_gather.relay()
    hidden_gather.arrive()

    def emit_expert(span, value):
        expert_out[span, :] = value.astype(expert_out.dtype)

    expert_sum.collect(emit_expert)
    for phase in (rows_gather, hidden_gather, dense_sum, expert_sum):
        phase.finish()


ROW_PIECES = 4


def branches(rows, every_cols, dense_gate, dense_up, gate, up, down, axis, size, collective_id):
    room, width = rows.shape
    total, hidden_width = every_cols.shape[0], dense_gate.shape[1]
    share, inner = total // size, gate.shape[1]
    fast = fast_extent(axis, size)
    slow = size // fast
    whole = pl.BlockSpec(memory_space=pltpu.VMEM)
    far = pl.BlockSpec(memory_space=pl.ANY)
    bf16 = jnp.bfloat16
    return pl.pallas_call(
        functools.partial(branches_kernel, axis, size),
        out_shape=(
            jax.ShapeDtypeStruct((size, share, hidden_width), bf16),
            jax.ShapeDtypeStruct((room, width), bf16),
        ),
        in_specs=[whole] * 4 + [far] * 3,
        out_specs=(whole, whole),
        scratch_shapes=[
            pltpu.VMEM((room, size * width), bf16),
            pltpu.VMEM(gate.shape, bf16),
            pltpu.VMEM(up.shape, bf16),
            pltpu.VMEM(down.shape, bf16),
            pltpu.VMEM((size, share, 2 * hidden_width), bf16),
            pltpu.VMEM((share, hidden_width), bf16),
            pltpu.VMEM((room, inner), bf16),
            pltpu.VMEM((room, size * width), bf16),
            pltpu.SemaphoreType.DMA((3,)),
        ]
        + gather_sems(fast, slow, ROW_PIECES)
        + gather_sems(fast, slow, 2)
        + reduce_scratch(fast, slow, share, 2 * hidden_width, 4)
        + reduce_scratch(fast, slow, room, width, 4),
        compiler_params=pltpu.CompilerParams(
            collective_id=collective_id, has_side_effects=True, vmem_limit_bytes=54 << 20
        ),
    )(rows, every_cols, dense_gate, dense_up, gate, up, down)


def rms_norm(values, gain):
    flt = values.astype(jnp.float32)
    scaled = flt * lax.rsqrt(jnp.mean(flt * flt, axis=-1, keepdims=True) + 1e-06)
    return (scaled * gain).astype(jnp.bfloat16)


def discretize(decay_rate, frequency, log_step, b_real, b_imag):
    step_size = jnp.exp(log_step)[:, None]
    lam_re = -decay_rate
    magnitude = jnp.exp(lam_re * step_size)
    abar_re = magnitude * jnp.cos(frequency * step_size)
    abar_im = magnitude * jnp.sin(frequency * step_size)
    denom = lam_re * lam_re + frequency * frequency
    fac_re = ((abar_re - 1.0) * lam_re + abar_im * frequency) / denom
    fac_im = (abar_im * lam_re - (abar_re - 1.0) * frequency) / denom
    bbar_re = fac_re[..., None] * b_real - fac_im[..., None] * b_imag
    bbar_im = fac_re[..., None] * b_imag + fac_im[..., None] * b_real
    return (abar_re, abar_im, bbar_re, bbar_im)


def state_step(
    drive, states, decay_rate, frequency, log_step, b_real, b_imag, c_real, c_imag, skip_gain
):
    count = drive.shape[0]
    groups = decay_rate.shape[0]
    abar_re, abar_im, bbar_re, bbar_im = discretize(decay_rate, frequency, log_step, b_real, b_imag)
    grouped = drive.astype(jnp.float32).reshape(count, groups, GROUP)
    old_re = states[0].reshape(count, groups, STATE)
    old_im = states[1].reshape(count, groups, STATE)
    high = lax.Precision.HIGHEST
    push_re = jnp.einsum("ngh,gph->ngp", grouped, bbar_re, precision=high)
    push_im = jnp.einsum("ngh,gph->ngp", grouped, bbar_im, precision=high)
    new_re = abar_re * old_re - abar_im * old_im + push_re
    new_im = abar_re * old_im + abar_im * old_re + push_im
    readout = (
        jnp.einsum("ngp,ghp->ngh", new_re, c_real, precision=high)
        - jnp.einsum("ngp,ghp->ngh", new_im, c_imag, precision=high)
        + skip_gain.reshape(groups, GROUP) * grouped
    )
    reads = jax.nn.gelu(readout.reshape(count, groups * GROUP)).astype(jnp.bfloat16)
    fresh = jnp.stack(
        [new_re.reshape(count, groups * STATE), new_im.reshape(count, groups * STATE)]
    )
    return (reads, fresh)


def shards(
    tokens,
    mix_gain,
    ffn_gain,
    in_proj,
    decay_rate,
    frequency,
    log_step,
    b_real,
    b_imag,
    c_real,
    c_imag,
    skip_gain,
    states,
    out_proj,
    route_ids,
    route_logits,
    expert_gate,
    expert_up,
    expert_down,
    dense_gate,
    dense_up,
    dense_down,
    branch_gate,
):
    seq_count, width = tokens.shape
    tp_count = lax.axis_size("tp")
    ep_count = lax.axis_size("ep")
    tp_index = lax.axis_index("tp")
    part_width = width // tp_count
    normed = rms_norm(tokens, mix_gain)
    drive = jnp.dot(normed, in_proj, preferred_element_type=jnp.float32).astype(jnp.bfloat16)
    reads, new_states = state_step(
        drive, states, decay_rate, frequency, log_step, b_real, b_imag, c_real, c_imag, skip_gain
    )
    partial_value = (
        jnp.dot(reads, out_proj, preferred_element_type=jnp.float32)
        .astype(jnp.bfloat16)
        .astype(jnp.float32)
    )
    mixed_cols = reduce_scatter(partial_value.astype(jnp.bfloat16), "tp", tp_count, 2, True, 0)
    (mixed,) = all_gather([mixed_cols], "tp", tp_count, [2], True, 1)
    resid = (tokens.astype(jnp.float32) + mixed.astype(jnp.float32)).astype(jnp.bfloat16)
    normed_two = rms_norm(resid, ffn_gain)
    own_cols = lax.dynamic_slice_in_dim(normed_two, tp_index * part_width, part_width, 1)
    branch = jax.nn.sigmoid(jnp.dot(normed_two, branch_gate, preferred_element_type=jnp.float32))
    route_weights = jax.nn.softmax(route_logits, axis=-1)
    top_count = route_ids.shape[1]
    side = jnp.concatenate(
        [route_ids.astype(jnp.float32).T, route_weights.T, branch[None, :]], axis=0
    )
    side = jnp.pad(side, ((0, -side.shape[0] % 8), (0, -seq_count % 128)))
    every_cols, every_side = all_gather([own_cols, side], "ep", ep_count, [2, 1], False, 2)
    total_count = ep_count * seq_count
    every_cols = every_cols.reshape(total_count, part_width)
    every_side = every_side[:, :, :seq_count].transpose(1, 0, 2).reshape(-1, total_count)
    every_ids = every_side[:top_count].T
    every_weights = every_side[top_count : 2 * top_count].T
    every_branch = every_side[2 * top_count]
    mine = every_ids == lax.axis_index("ep").astype(jnp.float32)
    taken = jnp.any(mine, axis=1)
    own_weight = jnp.sum(jnp.where(mine, every_weights, 0.0), axis=1)
    order = jnp.cumsum(taken.astype(jnp.int32)) - 1
    room = ep_count * max(2, 2 * seq_count * top_count // ep_count)
    slots = jnp.arange(room, dtype=jnp.int32)
    select = (order[None, :] == slots[:, None]) & taken[None, :]
    row_weight = jnp.sum(jnp.where(select, own_weight[None, :], 0.0), axis=1)
    select = select.astype(jnp.bfloat16)
    expert_in = jnp.dot(select, every_cols, preferred_element_type=jnp.float32).astype(jnp.bfloat16)
    dense_hidden, expert_cols = branches(
        expert_in,
        every_cols,
        dense_gate,
        dense_up,
        expert_gate[0],
        expert_up[0],
        expert_down[0],
        "tp",
        tp_count,
        3,
    )
    dense_hidden = dense_hidden.reshape(total_count, dense_gate.shape[1])
    weighted = (expert_cols.astype(jnp.float32) * row_weight[:, None]).astype(jnp.bfloat16)
    routed_part = lax.dot_general(
        select, weighted, (((0,), (0,)), ((), ())), preferred_element_type=jnp.float32
    )
    dense_part = jnp.dot(dense_hidden, dense_down, preferred_element_type=jnp.float32)
    share = (routed_part + every_branch[:, None] * dense_part).astype(jnp.bfloat16)
    share = share.reshape(ep_count, seq_count, part_width)
    gathered = reduce_scatter(share, "ep", ep_count, 2, False, 4)
    resid_cols = lax.dynamic_slice_in_dim(resid, tp_index * part_width, part_width, 1)
    output = (resid_cols.astype(jnp.float32) + gathered.astype(jnp.float32)).astype(jnp.bfloat16)
    return (output, new_states)


def solution(mesh):
    return jax.shard_map(
        shards,
        mesh=mesh,
        in_specs=(
            P("ep", None),
            P(),
            P(),
            P(None, "tp"),
            P("tp", None),
            P("tp", None),
            P("tp"),
            P("tp", None, None),
            P("tp", None, None),
            P("tp", None, None),
            P("tp", None, None),
            P("tp"),
            P(None, "ep", "tp"),
            P("tp", None),
            P("ep", None),
            P("ep", None),
            P("ep", None, "tp"),
            P("ep", None, "tp"),
            P("ep", "tp", None),
            P("tp", "ep"),
            P("tp", "ep"),
            P("ep", "tp"),
            P(),
        ),
        out_specs=(P("ep", "tp"), P(None, "ep", "tp")),
        check_vma=False,
    )
```
